32 devices in a mesh: kv: 8 (over z, y), tp: 4 (over x, core).
Axes of the slice: x: 2, y: 2, z: 4, core: 2. Of those that a mesh axis runs over, the one named last changes fastest.
Arguments:
- stream: bfloat16 [24, 4096], P(None, ('kv', 'tp')), may hold values from -50 to 50
- attention_gain: float32 [4096], P(('kv', 'tp')), may hold values from 0.1 to 1.9
- query_down: bfloat16 [4096, 1536], P(('kv', 'tp')), may hold values from -0.09375 to 0.09375
- latent_down: bfloat16 [4096, 512], P(('kv', 'tp')), may hold values from -0.09375 to 0.09375
- rotary_down: bfloat16 [4096, 64], P(('kv', 'tp')), may hold values from -0.1875 to 0.1875
- query_gain: float32 [1536], replicated, may hold values from 0.1 to 1.9
- latent_gain: float32 [512], replicated, may hold values from 0.1 to 1.9
- query_content: bfloat16 [1536, 2048], P(None, 'tp'), may hold values from -0.15625 to 0.15625
- query_rotary: bfloat16 [1536, 1024], P(None, 'tp'), may hold values from -0.15625 to 0.15625
- key_absorb: bfloat16 [16, 128, 512], P('tp'), may hold values from -0.5 to 0.5
- value_absorb: bfloat16 [16, 512, 128], P('tp'), may hold values from -0.25 to 0.25
- latent_cache: bfloat16 [24, 2048, 512], P(None, 'kv'), may hold values from -1200 to 1200
- rotary_cache: bfloat16 [24, 2048, 64], P(None, 'kv'), may hold values from -5 to 5
- head_gain: float32 [2048], P('tp'), may hold values from 0.1 to 1.9
- output_weight: bfloat16 [2048, 4096], P('tp', 'kv'), may hold values from -0.125 to 0.125
- mixer_gain: float32 [4096], P('kv'), may hold values from 0.1 to 1.9
- gate_weight: bfloat16 [4096, 11264], P('kv', 'tp'), may hold values from -0.09375 to 0.09375
- up_weight: bfloat16 [4096, 11264], P('kv', 'tp'), may hold values from -0.09375 to 0.09375
- down_weight: bfloat16 [11264, 4096], P('tp', 'kv'), may hold values from -0.0546875 to 0.0546875
Outputs:
- stream_out: bfloat16 [24, 4096], P(None, ('kv', 'tp'))
The draws below stay inside these ranges and needn't reach their ends.
All inputs are finite; a program needn't handle non-finite values.
Results may differ from the reference program's by a relative error of at most 0.018.
Values may be sent and summed in bfloat16 or wider, within the bound.
A program may use at most 64 MiB of HBM per device.

```python
import jax
import jax.numpy as jnp
from jax import lax

D = 4096
HEADS = 16
QRANK = 1536
KVRANK = 512
NOPE = 128
ROPE = 64
VDIM = 128
FF = 11264
SEQS = 24
POS_DEV = 256
LENGTH = 2048
N_KV = 8
N_TP = 4


def draw_stream(key, part):
    keys = jax.random.split(key, 3)
    columns = jnp.arange(D, dtype=jnp.float32) / D
    column_scale = jnp.exp(jnp.log(3.0) * columns + jax.random.uniform(keys[1], (1, D), jnp.float32, -0.35, 0.35))
    row_scale = jnp.exp(jax.random.uniform(keys[2], (SEQS, 1), jnp.float32, jnp.log(0.5), jnp.log(2.0)))
    entries = jax.random.truncated_normal(keys[0], -5.0, 5.0, (SEQS, D), jnp.float32)
    return (entries * row_scale * column_scale).astype(jnp.bfloat16)


def draw_latent_cache(key, part):
    keys = jax.random.split(key, 1)
    length = POS_DEV * N_KV
    base = 0.3 * jax.random.truncated_normal(keys[0], -5.0, 5.0, (SEQS, length, KVRANK), jnp.float32)
    return base.astype(jnp.bfloat16)


def block_scale(own_key, dims, pieces, low, top_value):
    factor_of, own = 1.0, jax.random.fold_in(own_key, 6)
    for dim, blocks in pieces:
        heights = jnp.exp(jax.random.uniform(jax.random.fold_in(own, dim), (blocks,), jnp.float32, low / len(pieces), top_value / len(pieces)))
        factor_of = factor_of * jnp.repeat(heights, dims[dim] // blocks).reshape([-1 if axis == dim else 1 for axis in range(len(dims))])
    return factor_of


def gaussian(stream_key, extent, scale, most, shards=(), held_as=jnp.bfloat16):
    array = scale * jax.random.normal(stream_key, extent, jnp.float32)
    if shards:
        array = array * block_scale(stream_key, extent, shards, -0.22, 0.18)
    return jnp.clip(array, -most, most).astype(held_as)


def setup_inputs(seed: int = 0) -> dict:
    streams_of = jax.random.split(jax.random.key(seed), 20)
    stream = draw_stream(jax.random.fold_in(streams_of[19], 71), 0)
    attention_gain = jnp.clip(1.0 + 0.18 * jax.random.normal(streams_of[1], (D,), jnp.float32), 0.1, 1.9)
    query_down = gaussian(streams_of[2], (D, QRANK), D ** -0.5, 0.09375, ((0, 32),))
    latent_down = gaussian(streams_of[3], (D, KVRANK), D ** -0.5, 0.09375, ((0, 32),))
    rotary_down = gaussian(streams_of[4], (D, ROPE), (D // 4) ** -0.5, 0.1875, ((0, 32),))
    query_gain = jnp.clip(1.0 + 0.18 * jax.random.normal(streams_of[5], (QRANK,), jnp.float32), 0.1, 1.9)
    latent_gain = jnp.clip(1.0 + 0.18 * jax.random.normal(streams_of[6], (KVRANK,), jnp.float32), 0.1, 1.9)
    query_content = gaussian(streams_of[7], (QRANK, HEADS * NOPE), QRANK ** -0.5, 0.15625, ((1, 4),))
    query_rotary = gaussian(streams_of[8], (QRANK, HEADS * ROPE), QRANK ** -0.5, 0.15625, ((1, 4),))
    key_absorb = gaussian(streams_of[9], (HEADS, NOPE, KVRANK), NOPE ** -0.5, 0.5, ((0, 4),))
    value_absorb = gaussian(streams_of[10], (HEADS, KVRANK, VDIM), KVRANK ** -0.5, 0.25, ((0, 4),))
    latent_cache = draw_latent_cache(jax.random.fold_in(streams_of[19], 71), 0)
    rotary_cache = gaussian(streams_of[12], (SEQS, LENGTH, ROPE), 1.0, 5.0, ((1, 8),))
    head_gain = jnp.clip(1.0 + 0.18 * jax.random.normal(streams_of[13], (HEADS * VDIM,), jnp.float32), 0.1, 1.9)
    output_weight = gaussian(streams_of[14], (HEADS * VDIM, D), (HEADS * VDIM) ** -0.5, 0.125, ((0, 4), (1, 8)))
    mixer_gain = jnp.clip(1.0 + 0.18 * jax.random.normal(streams_of[15], (D,), jnp.float32), 0.1, 1.9)
    gate_weight = gaussian(streams_of[16], (D, FF), D ** -0.5, 0.09375, ((0, 8), (1, 4)))
    up_weight = gaussian(streams_of[17], (D, FF), D ** -0.5, 0.09375, ((0, 8), (1, 4)))
    down_weight = gaussian(streams_of[18], (FF, D), FF ** -0.5, 0.0546875, ((0, 4), (1, 8)))
    return {"stream": stream, "attention_gain": attention_gain, "query_down": query_down, "latent_down": latent_down, "rotary_down": rotary_down, "query_gain": query_gain, "latent_gain": latent_gain, "query_content": query_content, "query_rotary": query_rotary, "key_absorb": key_absorb, "value_absorb": value_absorb, "latent_cache": latent_cache, "rotary_cache": rotary_cache, "head_gain": head_gain, "output_weight": output_weight, "mixer_gain": mixer_gain, "gate_weight": gate_weight, "up_weight": up_weight, "down_weight": down_weight}


epsilon = 1e-06
rope_base = 10000.0

def rotate(values, position):
    half = values.shape[-1] // 2
    freqs = rope_base ** (-jnp.arange(half, dtype=jnp.float32) * 2.0 / values.shape[-1])
    angle = position * freqs
    cosine = jnp.cos(angle)
    sine = jnp.sin(angle)
    first = values[..., :half]
    second = values[..., half:]
    return jnp.concatenate([first * cosine - second * sine, second * cosine + first * sine], axis=-1)

def inv_rms(values):
    return lax.rsqrt(lax.optimization_barrier(jnp.mean(values * values, axis=-1)) + epsilon)

def block_sum(left, right, parts):
    rows = left.shape[0]
    inner = right.shape[0] // parts
    terms = jnp.einsum('btf,tfd->btd', left.reshape(rows, parts, inner).astype(jnp.float32), right.reshape(parts, inner, right.shape[1]).astype(jnp.float32))
    rounded = lax.optimization_barrier(terms.astype(jnp.bfloat16))
    return lax.optimization_barrier(jnp.sum(rounded.astype(jnp.float32), axis=1))

def reference(stream, attention_gain, query_down, latent_down, rotary_down, query_gain, latent_gain, query_content, query_rotary, key_absorb, value_absorb, latent_cache, rotary_cache, head_gain, output_weight, mixer_gain, gate_weight, up_weight, down_weight):
    batch_rows = stream.shape[0]
    length = latent_cache.shape[1]
    position = jnp.float32(length)
    stream_f = stream.astype(jnp.float32)
    first_scale = inv_rms(stream_f)[:, None]
    first_scaled = (stream_f * attention_gain).astype(jnp.bfloat16)
    query_low = first_scale * jnp.dot(first_scaled, query_down, preferred_element_type=jnp.float32)
    latent_new = first_scale * jnp.dot(first_scaled, latent_down, preferred_element_type=jnp.float32)
    rotary_new = first_scale * jnp.dot(first_scaled, rotary_down, preferred_element_type=jnp.float32)
    query_normed = (query_low * inv_rms(query_low)[:, None] * query_gain).astype(jnp.bfloat16)
    latent_row = (latent_new * inv_rms(latent_new)[:, None] * latent_gain).astype(jnp.bfloat16)
    rotary_row = rotate(rotary_new, position).astype(jnp.bfloat16)
    heads = key_absorb.shape[0]
    query_plain = jnp.dot(query_normed, query_content, preferred_element_type=jnp.float32).astype(jnp.bfloat16)
    query_plain = query_plain.reshape(batch_rows, heads, key_absorb.shape[1])
    query_turned = jnp.dot(query_normed, query_rotary, preferred_element_type=jnp.float32)
    query_turned = rotate(query_turned.reshape(batch_rows, heads, rotary_cache.shape[2]), position).astype(jnp.bfloat16)
    query_latent = jnp.einsum('bhn,hnc->bhc', query_plain.astype(jnp.float32), key_absorb.astype(jnp.float32)).astype(jnp.bfloat16)
    scale = (key_absorb.shape[1] + rotary_cache.shape[2]) ** (-0.5)
    blocks = length // POS_DEV

    def one_sequence(items):
        row_latent, row_turned, latents, rotaries = items
        scores = (jnp.dot(row_latent, latents.T, preferred_element_type=jnp.float32) + jnp.dot(row_turned, rotaries.T, preferred_element_type=jnp.float32)) * scale
        scores = scores.reshape(heads, blocks, POS_DEV)
        maxima = lax.optimization_barrier(jnp.max(scores, axis=-1))
        expo = jnp.exp(scores - maxima[..., None])
        totals = lax.optimization_barrier(jnp.sum(expo, axis=-1))
        weights = expo.astype(jnp.bfloat16)
        weighted = jnp.einsum('hnp,npc->hnc', weights.astype(jnp.float32), latents.reshape(blocks, POS_DEV, latents.shape[1]).astype(jnp.float32))
        return (maxima, totals, weighted.astype(jnp.bfloat16))
    maxima, totals, weighted = lax.map(one_sequence, (query_latent, query_turned, latent_cache, rotary_cache))
    own_score = (lax.optimization_barrier(jnp.sum(query_latent.astype(jnp.float32) * latent_row.astype(jnp.float32)[:, None, :], axis=-1)) + lax.optimization_barrier(jnp.sum(query_turned.astype(jnp.float32) * rotary_row.astype(jnp.float32)[:, None, :], axis=-1))) * scale
    largest = jnp.maximum(lax.optimization_barrier(jnp.max(maxima, axis=-1)), own_score)
    factors = jnp.exp(maxima - largest[..., None])
    own_weight = jnp.exp(own_score - largest)
    denominator = lax.optimization_barrier(jnp.sum(factors * totals, axis=-1)) + own_weight
    merged = lax.optimization_barrier(jnp.sum(factors[..., None] * weighted.astype(jnp.float32), axis=2))
    merged = merged + own_weight[..., None] * latent_row.astype(jnp.float32)[:, None, :]
    latent_mix = (merged / denominator[..., None]).astype(jnp.bfloat16)
    head_values = jnp.einsum('bhc,hcv->bhv', latent_mix.astype(jnp.float32), value_absorb.astype(jnp.float32)).astype(jnp.bfloat16)
    head_f = head_values.reshape(batch_rows, heads * value_absorb.shape[2]).astype(jnp.float32)
    head_scale = inv_rms(head_f)[:, None]
    head_scaled = (head_f * head_gain).astype(jnp.bfloat16)
    attended = block_sum(head_scaled, output_weight, N_TP)
    middle = (stream_f + head_scale * attended).astype(jnp.bfloat16)
    middle_f = middle.astype(jnp.float32)
    second_scale = inv_rms(middle_f)[:, None]
    second_scaled = (middle_f * mixer_gain).astype(jnp.bfloat16)
    gate = second_scale * jnp.dot(second_scaled, gate_weight, preferred_element_type=jnp.float32)
    up = second_scale * jnp.dot(second_scaled, up_weight, preferred_element_type=jnp.float32)
    hidden = (jax.nn.silu(gate) * up).astype(jnp.bfloat16)
    mixed = block_sum(hidden, down_weight, N_TP)
    return (middle_f + mixed).astype(jnp.bfloat16)
```

```python
import functools

import jax
import jax.numpy as jnp
import numpy as np
from jax import lax
from jax.experimental import pallas as pl
from jax.experimental.pallas import tpu as pltpu
from jax.sharding import PartitionSpec as P

epsilon = 1e-06
rope_base = 10000.0


def rotate(values, position):
    half = values.shape[-1] // 2
    freqs = rope_base ** (-jnp.arange(half, dtype=jnp.float32) * 2.0 / values.shape[-1])
    angle = position * freqs
    cosine = jnp.cos(angle)
    sine = jnp.sin(angle)
    first = values[..., :half]
    second = values[..., half:]
    return jnp.concatenate(
        [first * cosine - second * sine, second * cosine + first * sine], axis=-1
    )


def inv_rms(values):
    return lax.rsqrt(jnp.mean(values * values, axis=-1) + epsilon)


def sum_squares(values):
    return jnp.sum(values * values, axis=-1)


def matmul(left, right):
    return jnp.dot(left, right, preferred_element_type=jnp.float32)


def local(
    stream,
    attention_gain,
    query_down,
    latent_down,
    rotary_down,
    query_gain,
    latent_gain,
    query_content,
    query_rotary,
    key_absorb,
    value_absorb,
    latent_cache,
    rotary_cache,
    head_gain,
    output_weight,
    mixer_gain,
    gate_weight,
    up_weight,
    down_weight,
):
    kv_count = lax.axis_size("kv")
    tp_count = lax.axis_size("tp")
    batch_rows = stream.shape[0]
    model_width = stream.shape[1] * kv_count * tp_count
    position = jnp.float32(latent_cache.shape[1] * kv_count)
    stream_block = lax.all_gather(stream, "tp", axis=1, tiled=True)
    stream_f = stream.astype(jnp.float32)
    first_scaled = (stream_f * attention_gain).astype(jnp.bfloat16)
    query_sum, latent_sum, rotary_sum, square_sum = lax.psum(
        (
            matmul(first_scaled, query_down),
            matmul(first_scaled, latent_down),
            matmul(first_scaled, rotary_down),
            sum_squares(stream_f),
        ),
        ("kv", "tp"),
    )
    first_scale = lax.rsqrt(square_sum / model_width + epsilon)[:, None]
    query_low = first_scale * query_sum
    latent_new = first_scale * latent_sum
    rotary_new = first_scale * rotary_sum
    query_normed = (query_low * inv_rms(query_low)[:, None] * query_gain).astype(jnp.bfloat16)
    latent_row = (latent_new * inv_rms(latent_new)[:, None] * latent_gain).astype(jnp.bfloat16)
    rotary_row = rotate(rotary_new, position).astype(jnp.bfloat16)
    heads_here = key_absorb.shape[0]
    query_plain = matmul(query_normed, query_content).astype(jnp.bfloat16)
    query_plain = query_plain.reshape(batch_rows, heads_here, key_absorb.shape[1])
    query_turned = matmul(query_normed, query_rotary).reshape(
        batch_rows, heads_here, rotary_cache.shape[2]
    )
    query_turned = rotate(query_turned, position).astype(jnp.bfloat16)
    query_latent = jnp.einsum(
        "bhn,hnc->bhc", query_plain, key_absorb, preferred_element_type=jnp.float32
    ).astype(jnp.bfloat16)
    scale = (key_absorb.shape[1] + rotary_cache.shape[2]) ** (-0.5)
    scores = (
        jnp.einsum("bhc,bpc->bhp", query_latent, latent_cache, preferred_element_type=jnp.float32)
        + jnp.einsum("bhr,bpr->bhp", query_turned, rotary_cache, preferred_element_type=jnp.float32)
    ) * scale
    maxima = jnp.max(scores, axis=-1)
    expo = jnp.exp(scores - maxima[..., None])
    totals = jnp.sum(expo, axis=-1)
    weighted = jnp.einsum(
        "bhp,bpc->bhc", expo.astype(jnp.bfloat16), latent_cache, preferred_element_type=jnp.float32
    ).astype(jnp.bfloat16)
    all_maxima, all_totals = (
        lax.all_gather(maxima[None], "kv", axis=0, tiled=True),
        lax.all_gather(totals[None], "kv", axis=0, tiled=True),
    )
    own_score = (
        jnp.sum(
            query_latent.astype(jnp.float32) * latent_row.astype(jnp.float32)[:, None, :], axis=-1
        )
        + jnp.sum(
            query_turned.astype(jnp.float32) * rotary_row.astype(jnp.float32)[:, None, :], axis=-1
        )
    ) * scale
    largest = jnp.maximum(jnp.max(all_maxima, axis=0), own_score)
    factors = jnp.exp(all_maxima - largest[None])
    own_weight = jnp.exp(own_score - largest)
    denominator = jnp.sum(factors * all_totals, axis=0) + own_weight
    merged = jnp.sum(
        factors[..., None]
        * lax.all_gather(weighted[None], "kv", axis=0, tiled=True).astype(jnp.float32),
        axis=0,
    )
    merged = merged + own_weight[..., None] * latent_row.astype(jnp.float32)[:, None, :]
    latent_mix = (merged / denominator[..., None]).astype(jnp.bfloat16)
    head_values = jnp.einsum(
        "bhc,hcv->bhv", latent_mix, value_absorb, preferred_element_type=jnp.float32
    ).astype(jnp.bfloat16)
    head_f = head_values.reshape(batch_rows, heads_here * value_absorb.shape[2]).astype(jnp.float32)
    head_square = lax.psum(sum_squares(head_f), "tp")
    head_scale = lax.rsqrt(head_square / (head_f.shape[1] * tp_count) + epsilon)[:, None]
    head_scaled = (head_f * head_gain).astype(jnp.bfloat16)
    attended = lax.psum(matmul(head_scaled, output_weight).astype(jnp.bfloat16), "tp").astype(
        jnp.float32
    )
    middle = (stream_block.astype(jnp.float32) + head_scale * attended).astype(jnp.bfloat16)
    middle_f = middle.astype(jnp.float32)
    second_scaled = (middle_f * mixer_gain).astype(jnp.bfloat16)
    gate_part = matmul(second_scaled, gate_weight)
    up_part = matmul(second_scaled, up_weight)
    gate_total, up_total, middle_square = (
        lax.psum(gate_part.astype(jnp.bfloat16), "kv").astype(jnp.float32),
        lax.psum(up_part.astype(jnp.bfloat16), "kv").astype(jnp.float32),
        lax.psum(sum_squares(middle_f).astype(jnp.bfloat16), "kv").astype(jnp.float32),
    )
    second_scale = lax.rsqrt(middle_square / model_width + epsilon)[:, None]
    hidden = (jax.nn.silu(second_scale * gate_total) * (second_scale * up_total)).astype(
        jnp.bfloat16
    )
    mixed = lax.psum_scatter(
        matmul(hidden, down_weight).astype(jnp.bfloat16), "tp", scatter_dimension=1, tiled=True
    ).astype(jnp.float32)
    share_width = mixed.shape[1]
    own_middle = lax.dynamic_slice_in_dim(
        middle_f, lax.axis_index("tp") * share_width, share_width, 1
    )
    return (own_middle + mixed).astype(jnp.bfloat16)


LANES = 128
SUBLANES = 8
MESH = pl.DeviceIdType.MESH


def ceil_div(value, step):
    return -(-value // step)


def tables(width, count, position):
    half = width // 2
    freqs = rope_base ** (-np.arange(half, dtype=np.float64) * 2.0 / width)
    angle = position * freqs
    cosine = np.concatenate([np.cos(angle), np.cos(angle)])
    sine = np.concatenate([-np.sin(angle), np.sin(angle)])
    return (
        np.tile(cosine, count)[None].astype(np.float32),
        np.tile(sine, count)[None].astype(np.float32),
    )


def turned(values, cosine, sine, width):
    lanes = values.shape[1]
    half = width // 2
    lane = lax.broadcasted_iota(jnp.int32, values.shape, 1)
    ahead = pltpu.roll(values, lanes - half, 1)
    behind = pltpu.roll(values, half, 1)
    swapped = jnp.where(lax.rem(lane, width) < half, ahead, behind)
    return values * cosine + swapped * sine


def matmul_nt(left, right):
    return lax.dot_general(
        left, right, (((1,), (1,)), ((), ())), preferred_element_type=jnp.float32
    )


def fused(
    n_kv,
    n_tp,
    dims,
    stream_ref,
    attention_gain,
    query_gain,
    latent_gain,
    head_gain,
    mixer_gain,
    cos_ref,
    sin_ref,
    *refs,
):
    rows, depth, qrank, kvrank, rope, nope, vdim, heads, hidden_width, block_width, share, positions = dims
    hbm = refs[:13]
    out_ref = refs[13]
    vmem = refs[14:27]
    (
        load_sems,
        tp_sems,
        kv_sems,
        stream_all,
        a_send,
        a_recv,
        a_sum,
        a_part,
        a_total,
        a_all,
        q_lat,
        q_rot,
        own_lat,
        own_stat,
        own_rows,
        s_ref,
        e_ref,
        w_ref,
        w_send,
        w_recv,
        st_send,
        st_recv,
        hv_send,
        hv_recv,
        hv_rows,
        o_recv,
        osq_recv,
        o_send,
        osq_send,
        mid_ref,
        d_send,
        d_recv,
        dsq_send,
        dsq_recv,
        h_all,
        h_send,
        e_send,
        e_recv,
    ) = refs[27:]
    (
        qd_v,
        ld_v,
        rd_v,
        qc_v,
        qr_v,
        ka_v,
        lat_v,
        rot_v,
        va_v,
        ow_v,
        gate_v,
        up_v,
        down_v,
    ) = vmem
    kv = lax.axis_index("kv")
    tp = lax.axis_index("tp")
    model_width = block_width * n_kv

    loads = []
    for index, (source, target) in enumerate(zip(hbm, vmem)):
        if index in (10, 11):
            target = target.at[:, pl.ds(0, hidden_width)]
        elif index == 12:
            target = target.at[pl.ds(0, hidden_width)]
        copy = pltpu.make_async_copy(source, target, load_sems.at[index])
        copy.start()
        loads.append(copy)

    barrier = pltpu.get_barrier_semaphore()
    for d in range(1, n_tp):
        pl.semaphore_signal(
            barrier, inc=1, device_id=(kv, lax.rem(tp + d, n_tp)), device_id_type=MESH
        )
    for d in range(1, n_kv):
        pl.semaphore_signal(
            barrier, inc=1, device_id=(lax.rem(kv + d, n_kv), tp), device_id_type=MESH
        )

    sent = []

    def send(axis, stage, d, source, target):
        if axis == "tp":
            peer, sems = (kv, lax.rem(tp + d, n_tp)), tp_sems
        else:
            peer, sems = (lax.rem(kv + d, n_kv), tp), kv_sems
        copy = pltpu.make_async_remote_copy(
            src_ref=source,
            dst_ref=target,
            send_sem=sems.at[stage, 0, d - 1],
            recv_sem=sems.at[stage, 1, d - 1],
            device_id=peer,
            device_id_type=MESH,
        )
        copy.start()
        sent.append(copy)
        return copy

    def arrive(copies):
        for copy in copies:
            copy.wait_recv()

    pad = gate_v.shape[1] - hidden_width
    if pad:
        gate_v[:, hidden_width:] = jnp.zeros((block_width, pad), gate_v.dtype)
        up_v[:, hidden_width:] = jnp.zeros((block_width, pad), up_v.dtype)
        down_v[hidden_width:, :] = jnp.zeros((pad, block_width), down_v.dtype)

    stream_f = stream_ref[...].astype(jnp.float32)
    first_scaled = (stream_f * attention_gain[...]).astype(jnp.bfloat16)
    for index in range(3):
        loads[index].wait()
    parts = [matmul(first_scaled, qd_v[...]), matmul(first_scaled, ld_v[...])]
    rotary_part = matmul(first_scaled, rd_v[...])
    square = jnp.sum(stream_f * stream_f, axis=1, keepdims=True)
    last = jnp.concatenate(
        [rotary_part, jnp.broadcast_to(square, (rows, LANES - rope))], axis=1
    )
    tiles = []
    for part in parts:
        for j in range(part.shape[1] // LANES):
            tiles.append(part[:, j * LANES : (j + 1) * LANES])
    tiles.append(last)
    row_tiles = rows // SUBLANES
    blocks = a_send.shape[1]
    per_kv = blocks // n_kv
    for t in range(n_tp):
        for i in range(blocks):
            k, r = divmod(i, row_tiles)
            j = k * n_tp + t
            if j < len(tiles):
                a_send[t, i] = tiles[j][r * SUBLANES : (r + 1) * SUBLANES]
            else:
                a_send[t, i] = jnp.zeros((SUBLANES, LANES), jnp.float32)
    pl.semaphore_wait(barrier, n_tp - 1 + n_kv - 1)
    copies = [
        send("tp", 1, d, a_send.at[lax.rem(tp + d, n_tp)], a_recv.at[tp]) for d in range(1, n_tp)
    ]
    stream_copies = [send("tp", 0, d, stream_ref, stream_all.at[tp]) for d in range(1, n_tp)]
    stream_all[tp] = stream_ref[...]
    a_recv[tp] = a_send[tp]
    arrive(copies)
    total = a_recv[0]
    for t in range(1, n_tp):
        total = total + a_recv[t]
    a_sum[...] = total
    copies = [
        send(
            "kv",
            0,
            d,
            a_sum.at[pl.ds(lax.rem(kv + d, n_kv) * per_kv, per_kv)],
            a_part.at[kv],
        )
        for d in range(1, n_kv)
    ]
    a_part[kv] = a_sum[pl.ds(kv * per_kv, per_kv)]
    arrive(copies)
    total = a_part[0]
    for p in range(1, n_kv):
        total = total + a_part[p]
    a_total[pl.ds(kv * per_kv, per_kv)] = total
    mine = a_total.at[pl.ds(kv * per_kv, per_kv)]
    arrive([send("kv", 1, d, mine, mine) for d in range(1, n_kv)])
    copies = [send("tp", 2, d, a_total, a_all.at[tp]) for d in range(1, n_tp)]
    a_all[tp] = a_total[...]
    arrive(copies)

    def tile_of(j):
        k, t = divmod(j, n_tp)
        return jnp.concatenate([a_all[t, k * row_tiles + r] for r in range(row_tiles)], axis=0)

    q_tiles, l_tiles = qrank // LANES, kvrank // LANES
    last = tile_of(q_tiles + l_tiles)
    first_scale = lax.rsqrt(last[:, rope : rope + 1] / model_width + epsilon)
    query_low = first_scale * jnp.concatenate([tile_of(j) for j in range(q_tiles)], axis=1)
    latent_new = first_scale * jnp.concatenate(
        [tile_of(q_tiles + j) for j in range(l_tiles)], axis=1
    )

    def normed(values, gain):
        mean = jnp.sum(values * values, axis=1, keepdims=True) / values.shape[1]
        return (values * lax.rsqrt(mean + epsilon) * gain).astype(jnp.bfloat16)

    query_normed = normed(query_low, query_gain[...])
    latent_row = normed(latent_new, latent_gain[...]).astype(jnp.float32)
    lane = lax.broadcasted_iota(jnp.int32, (rows, LANES), 1)
    cosine, sine = cos_ref[...], sin_ref[...]
    rotary_row = turned(first_scale * last, cosine[:, :LANES], sine[:, :LANES], rope)
    rotary_row = jnp.where(lane < rope, rotary_row, 0.0).astype(jnp.bfloat16).astype(jnp.float32)

    loads[3].wait()
    query_plain = matmul(query_normed, qc_v[...]).astype(jnp.bfloat16)
    loads[4].wait()
    query_turned = turned(matmul(query_normed, qr_v[...]), cosine, sine, rope)
    query_turned = query_turned.astype(jnp.bfloat16).astype(jnp.float32)
    loads[5].wait()
    scale = (nope + rope) ** (-0.5)
    per_tile = LANES // rope
    for h in range(heads):
        row = pl.ds(h, rows, stride=heads)
        latent = matmul(query_plain[:, h * nope : (h + 1) * nope], ka_v[h])
        latent = latent.astype(jnp.bfloat16).astype(jnp.float32)
        tile = h // per_tile
        rotary = query_turned[:, tile * LANES : (tile + 1) * LANES]
        shift = (h % per_tile) * rope
        if shift:
            rotary = pltpu.roll(rotary, LANES - shift, 1)
        rotary = jnp.where(lane < rope, rotary, 0.0)
        own = (
            jnp.sum(latent * latent_row, axis=1, keepdims=True)
            + jnp.sum(rotary * rotary_row, axis=1, keepdims=True)
        ) * scale
        for c in range(l_tiles):
            q_lat[c, row, :] = latent[:, c * LANES : (c + 1) * LANES]
            own_lat[c, row, :] = latent_row[:, c * LANES : (c + 1) * LANES]
        q_rot[row, :] = rotary
        own_stat[row, :] = jnp.broadcast_to(own, (rows, LANES))

    group = SUBLANES // heads
    steps = rows // group
    unroll = 3 if steps % 3 == 0 else 1
    sub_row = lax.broadcasted_iota(jnp.int32, (SUBLANES, 1), 0) // heads
    loads[6].wait()
    loads[7].wait()

    def score_step(outer, carry):
        for inner in range(unroll):
            i = outer * unroll + inner
            at = pl.ds(pl.multiple_of(i * SUBLANES, SUBLANES), SUBLANES)
            query = jnp.concatenate([q_lat[c, at, :] for c in range(l_tiles)], axis=1).astype(
                jnp.bfloat16
            )
            rotary = q_rot[at, :][:, :rope].astype(jnp.bfloat16)
            result = None
            for s in range(group):
                b = i * group + s
                score = matmul_nt(query, lat_v[b]) + matmul_nt(rotary, rot_v[b])
                result = score if s == 0 else jnp.where(sub_row == s, score, result)
            s_ref[at, :] = result * scale
        return carry

    lax.fori_loop(0, steps // unroll, score_step, 0)
    scores = s_ref[...]
    maxima = jnp.max(scores, axis=1, keepdims=True)
    expo = jnp.exp(scores - maxima)
    totals = jnp.sum(expo, axis=1, keepdims=True)
    e_ref[...] = expo
    all_rows = rows * heads
    own_rows_count = all_rows // n_kv
    stat_lane = lax.broadcasted_iota(jnp.int32, (all_rows, LANES), 1)
    stats = jnp.where(stat_lane < LANES // 2, maxima, totals)
    for p in range(n_kv):
        st_send[p] = stats[p * own_rows_count : (p + 1) * own_rows_count]
    stat_copies = [
        send("kv", 2, d, st_send.at[lax.rem(kv + d, n_kv)], st_recv.at[kv])
        for d in range(1, n_kv)
    ]
    st_recv[kv] = st_send[kv]

    def weight_step(outer, carry):
        for inner in range(unroll):
            i = outer * unroll + inner
            at = pl.ds(pl.multiple_of(i * SUBLANES, SUBLANES), SUBLANES)
            weights = e_ref[at, :].astype(jnp.bfloat16)
            result = None
            for s in range(group):
                value = matmul(weights, lat_v[i * group + s])
                result = value if s == 0 else jnp.where(sub_row == s, value, result)
            w_ref[at, :] = result
        return carry

    lax.fori_loop(0, steps // unroll, weight_step, 0)
    for p in range(n_kv):
        own = slice(p * own_rows_count, (p + 1) * own_rows_count)
        w_send[p] = w_ref[own, :].astype(jnp.bfloat16)
        for c in range(l_tiles):
            own_rows[p, :, c * LANES : (c + 1) * LANES] = own_lat[c, own, :]
        own_rows[p, :, kvrank:] = own_stat[own, :]
    copies = [
        send("kv", 3, d, w_send.at[lax.rem(kv + d, n_kv)], w_recv.at[kv]) for d in range(1, n_kv)
    ]
    w_recv[kv] = w_send[kv]
    own = own_rows[kv]
    own_score = own[:, kvrank : kvrank + 1]
    arrive(stat_copies)
    stat = [st_recv[p] for p in range(n_kv)]
    largest = own_score
    for p in range(n_kv):
        largest = jnp.maximum(largest, stat[p][:, 0:1])
    own_weight = jnp.exp(own_score - largest)
    denominator = own_weight
    factors = []
    for p in range(n_kv):
        factor = jnp.exp(stat[p][:, 0:1] - largest)
        factors.append(factor)
        denominator = denominator + factor * stat[p][:, LANES // 2 : LANES // 2 + 1]
    arrive(copies)
    merged = own_weight * own[:, :kvrank]
    for p in range(n_kv):
        merged = merged + factors[p] * w_recv[p].astype(jnp.float32)
    latent_mix = (merged / denominator).astype(jnp.bfloat16)
    loads[8].wait()
    head_row = lax.rem(lax.broadcasted_iota(jnp.int32, (own_rows_count, 1), 0), heads)
    values = None
    for h in range(heads):
        value = matmul(latent_mix, va_v[h])
        values = value if h == 0 else jnp.where(head_row == h, value, values)
    values = values.astype(jnp.bfloat16).astype(jnp.float32)
    hv_send[...] = values
    copies = [send("kv", 4, d, hv_send, hv_recv.at[kv]) for d in range(1, n_kv)]
    hv_recv[kv] = values
    arrive(copies)
    for p in range(n_kv):
        hv_rows[p * own_rows_count : (p + 1) * own_rows_count, :] = hv_recv[p]
    head_f = jnp.concatenate(
        [hv_rows[pl.ds(h, rows, stride=heads), :] for h in range(heads)], axis=1
    )
    head_square = jnp.sum(head_f * head_f, axis=1, keepdims=True)
    head_scaled = (head_f * head_gain[...]).astype(jnp.bfloat16)
    osq_send[...] = jnp.broadcast_to(head_square, (rows, LANES))
    square_copies = [send("tp", 3, d, osq_send, osq_recv.at[tp]) for d in range(1, n_tp)]
    osq_recv[tp] = osq_send[...]
    loads[9].wait()
    o_send[...] = matmul(head_scaled, ow_v[...]).astype(jnp.bfloat16)
    copies = [send("tp", 4, d, o_send, o_recv.at[tp]) for d in range(1, n_tp)]
    o_recv[tp] = o_send[...]
    arrive(stream_copies)
    stream_block = jnp.concatenate([stream_all[t] for t in range(n_tp)], axis=1).astype(
        jnp.float32
    )
    arrive(square_copies)
    square = osq_recv[0]
    for t in range(1, n_tp):
        square = square + osq_recv[t]
    head_scale = lax.rsqrt(square[:, 0:1] / (heads * vdim * n_tp) + epsilon)
    arrive(copies)
    attended = o_recv[0].astype(jnp.float32)
    for t in range(1, n_tp):
        attended = attended + o_recv[t].astype(jnp.float32)
    middle = (stream_block + head_scale * attended).astype(jnp.bfloat16).astype(jnp.float32)
    for t in range(n_tp):
        mid_ref[t] = middle[:, t * share : (t + 1) * share]

    dsq_send[...] = jnp.broadcast_to(
        jnp.sum(middle * middle, axis=1, keepdims=True), (rows, LANES)
    )
    square_copies = [send("kv", 5, d, dsq_send, dsq_recv.at[kv]) for d in range(1, n_kv)]
    dsq_recv[kv] = dsq_send[...]
    second_scaled = (middle * mixer_gain[...]).astype(jnp.bfloat16)
    loads[10].wait()
    loads[11].wait()
    chunk = gate_v.shape[1] // n_kv
    copies = []
    for d in list(range(1, n_kv)) + [0]:
        peer = lax.rem(kv + d, n_kv)
        columns = pl.ds(pl.multiple_of(peer * chunk, LANES), chunk)
        gate = matmul(second_scaled, gate_v[:, columns]).astype(jnp.bfloat16)
        up = matmul(second_scaled, up_v[:, columns]).astype(jnp.bfloat16)
        if d:
            d_send[peer, :, :chunk] = gate
            d_send[peer, :, chunk:] = up
            copies.append(send("kv", 6, d, d_send.at[peer], d_recv.at[kv]))
        else:
            d_recv[kv, :, :chunk] = gate
            d_recv[kv, :, chunk:] = up
    arrive(square_copies)
    square = dsq_recv[0]
    for p in range(1, n_kv):
        square = square + dsq_recv[p]
    second_scale = lax.rsqrt(square[:, 0:1] / model_width + epsilon)
    arrive(copies)
    total = d_recv[0].astype(jnp.float32)
    for p in range(1, n_kv):
        total = total + d_recv[p].astype(jnp.float32)
    gate = second_scale * total[:, :chunk]
    up = second_scale * total[:, chunk:]
    h_send[...] = (gate / (1.0 + jnp.exp(-gate)) * up).astype(jnp.bfloat16)
    copies = [send("kv", 7, d, h_send, h_all.at[kv]) for d in range(1, n_kv)]
    loads[12].wait()
    mixed = matmul(h_send[...], down_v[pl.ds(pl.multiple_of(kv * chunk, LANES), chunk), :])
    for d in range(1, n_kv):
        copies[d - 1].wait_recv()
        peer = lax.rem(kv + n_kv - d, n_kv)
        mixed = mixed + matmul(
            h_all[peer], down_v[pl.ds(pl.multiple_of(peer * chunk, LANES), chunk), :]
        )
    for t in range(n_tp):
        e_send[t] = mixed[:, t * share : (t + 1) * share].astype(jnp.bfloat16)
    copies = [
        send("tp", 5, d, e_send.at[lax.rem(tp + d, n_tp)], e_recv.at[tp]) for d in range(1, n_tp)
    ]
    e_recv[tp] = e_send[tp]
    arrive(copies)
    total = e_recv[0].astype(jnp.float32)
    for t in range(1, n_tp):
        total = total + e_recv[t].astype(jnp.float32)
    out_ref[...] = (mid_ref[tp] + total).astype(jnp.bfloat16)
    for copy in sent:
        copy.wait_send()


def layer(
    n_kv,
    n_tp,
    stream,
    attention_gain,
    query_down,
    latent_down,
    rotary_down,
    query_gain,
    latent_gain,
    query_content,
    query_rotary,
    key_absorb,
    value_absorb,
    latent_cache,
    rotary_cache,
    head_gain,
    output_weight,
    mixer_gain,
    gate_weight,
    up_weight,
    down_weight,
):
    rows, share = stream.shape
    heads, nope, kvrank = key_absorb.shape
    vdim = value_absorb.shape[2]
    qrank = query_down.shape[1]
    rope = rotary_down.shape[1]
    positions = latent_cache.shape[1]
    block_width, hidden_width = gate_weight.shape
    aligned = (
        all(
            size % LANES == 0
            for size in (share, qrank, kvrank, nope, vdim, positions, hidden_width)
        )
        and rope < LANES
        and LANES % rope == 0
        and (heads * rope) % LANES == 0
        and rows % SUBLANES == 0
        and SUBLANES % heads == 0
        and rows % (SUBLANES // heads) == 0
        and rows % n_kv == 0
        and n_kv > 1
        and n_tp > 1
    )
    if not aligned:
        return local(
            stream,
            attention_gain,
            query_down,
            latent_down,
            rotary_down,
            query_gain,
            latent_gain,
            query_content,
            query_rotary,
            key_absorb,
            value_absorb,
            latent_cache,
            rotary_cache,
            head_gain,
            output_weight,
            mixer_gain,
            gate_weight,
            up_weight,
            down_weight,
        )
    dims = (rows, share, qrank, kvrank, rope, nope, vdim, heads, hidden_width, block_width, share, positions)
    cosine, sine = tables(rope, heads, positions * n_kv)
    n_tiles = qrank // LANES + kvrank // LANES + 1
    blocks = ceil_div(ceil_div(n_tiles, n_tp) * (rows // SUBLANES), n_kv) * n_kv
    chunk = ceil_div(ceil_div(hidden_width, LANES), n_kv) * LANES
    all_rows = rows * heads
    own = all_rows // n_kv
    l_tiles = kvrank // LANES
    bf16, f32 = jnp.bfloat16, jnp.float32
    big = (
        query_down,
        latent_down,
        rotary_down,
        query_content,
        query_rotary,
        key_absorb,
        latent_cache,
        rotary_cache,
        value_absorb,
        output_weight,
        gate_weight,
        up_weight,
        down_weight,
    )
    held = [pltpu.VMEM(array.shape, array.dtype) for array in big]
    held[10] = held[11] = pltpu.VMEM((block_width, chunk * n_kv), bf16)
    held[12] = pltpu.VMEM((chunk * n_kv, block_width), bf16)
    scratch = held + [
        pltpu.SemaphoreType.DMA((len(big),)),
        pltpu.SemaphoreType.DMA((6, 2, n_tp - 1)),
        pltpu.SemaphoreType.DMA((8, 2, n_kv - 1)),
        pltpu.VMEM((n_tp, rows, share), bf16),
        pltpu.VMEM((n_tp, blocks, SUBLANES, LANES), f32),
        pltpu.VMEM((n_tp, blocks, SUBLANES, LANES), f32),
        pltpu.VMEM((blocks, SUBLANES, LANES), f32),
        pltpu.VMEM((n_kv, blocks // n_kv, SUBLANES, LANES), f32),
        pltpu.VMEM((blocks, SUBLANES, LANES), f32),
        pltpu.VMEM((n_tp, blocks, SUBLANES, LANES), f32),
        pltpu.VMEM((l_tiles, all_rows, LANES), f32),
        pltpu.VMEM((all_rows, LANES), f32),
        pltpu.VMEM((l_tiles, all_rows, LANES), f32),
        pltpu.VMEM((all_rows, LANES), f32),
        pltpu.VMEM((n_kv, own, kvrank + LANES), f32),
        pltpu.VMEM((all_rows, positions), f32),
        pltpu.VMEM((all_rows, positions), f32),
        pltpu.VMEM((all_rows, kvrank), f32),
        pltpu.VMEM((n_kv, own, kvrank), bf16),
        pltpu.VMEM((n_kv, own, kvrank), bf16),
        pltpu.VMEM((n_kv, own, LANES), f32),
        pltpu.VMEM((n_kv, own, LANES), f32),
        pltpu.VMEM((own, vdim), f32),
        pltpu.VMEM((n_kv, own, vdim), f32),
        pltpu.VMEM((all_rows, vdim), f32),
        pltpu.VMEM((n_tp, rows, block_width), bf16),
        pltpu.VMEM((n_tp, rows, LANES), f32),
        pltpu.VMEM((rows, block_width), bf16),
        pltpu.VMEM((rows, LANES), f32),
        pltpu.VMEM((n_tp, rows, share), f32),
        pltpu.VMEM((n_kv, rows, 2 * chunk), bf16),
        pltpu.VMEM((n_kv, rows, 2 * chunk), bf16),
        pltpu.VMEM((rows, LANES), f32),
        pltpu.VMEM((n_kv, rows, LANES), f32),
        pltpu.VMEM((n_kv, rows, chunk), bf16),
        pltpu.VMEM((rows, chunk), bf16),
        pltpu.VMEM((n_tp, rows, share), bf16),
        pltpu.VMEM((n_tp, rows, share), bf16),
    ]
    vmem = pl.BlockSpec(memory_space=pltpu.VMEM)
    return pl.pallas_call(
        functools.partial(fused, n_kv, n_tp, dims),
        out_shape=jax.ShapeDtypeStruct(stream.shape, stream.dtype),
        in_specs=[vmem] * 8 + [pl.BlockSpec(memory_space=pl.ANY)] * len(big),
        out_specs=vmem,
        scratch_shapes=scratch,
        compiler_params=pltpu.CompilerParams(
            collective_id=0, has_side_effects=True, vmem_limit_bytes=64000000
        ),
        name="layer",
    )(
        stream,
        attention_gain[None],
        query_gain[None],
        latent_gain[None],
        head_gain[None],
        mixer_gain[None],
        cosine,
        sine,
        *big,
    )


def solution(mesh):
    return jax.shard_map(
        functools.partial(layer, mesh.shape["kv"], mesh.shape["tp"]),
        mesh=mesh,
        in_specs=(
            P(None, ("kv", "tp")),
            P(("kv", "tp")),
            P(("kv", "tp"), None),
            P(("kv", "tp"), None),
            P(("kv", "tp"), None),
            P(),
            P(),
            P(None, "tp"),
            P(None, "tp"),
            P("tp", None, None),
            P("tp", None, None),
            P(None, "kv", None),
            P(None, "kv", None),
            P("tp"),
            P("tp", "kv"),
            P("kv"),
            P("kv", "tp"),
            P("kv", "tp"),
            P("tp", "kv"),
        ),
        out_specs=P(None, ("kv", "tp")),
        check_vma=False,
    )
```

```python
import functools

import jax
import jax.numpy as jnp
import numpy as np
from jax import lax
from jax.experimental import pallas as pl
from jax.experimental.pallas import tpu as pltpu
from jax.sharding import PartitionSpec as P

epsilon = 1e-06
rope_base = 10000.0


def rotate(values, position):
    half = values.shape[-1] // 2
    freqs = rope_base ** (-jnp.arange(half, dtype=jnp.float32) * 2.0 / values.shape[-1])
    angle = position * freqs
    cosine = jnp.cos(angle)
    sine = jnp.sin(angle)
    first = values[..., :half]
    second = values[..., half:]
    return jnp.concatenate(
        [first * cosine - second * sine, second * cosine + first * sine], axis=-1
    )


def inv_rms(values):
    return lax.rsqrt(jnp.mean(values * values, axis=-1) + epsilon)


def sum_squares(values):
    return jnp.sum(values * values, axis=-1)


def matmul(left, right):
    return jnp.dot(left, right, preferred_element_type=jnp.float32)


def local(
    stream,
    attention_gain,
    query_down,
    latent_down,
    rotary_down,
    query_gain,
    latent_gain,
    query_content,
    query_rotary,
    key_absorb,
    value_absorb,
    latent_cache,
    rotary_cache,
    head_gain,
    output_weight,
    mixer_gain,
    gate_weight,
    up_weight,
    down_weight,
):
    kv_count = lax.axis_size("kv")
    tp_count = lax.axis_size("tp")
    batch_rows = stream.shape[0]
    model_width = stream.shape[1] * kv_count * tp_count
    position = jnp.float32(latent_cache.shape[1] * kv_count)
    stream_block = lax.all_gather(stream, "tp", axis=1, tiled=True)
    stream_f = stream.astype(jnp.float32)
    first_scaled = (stream_f * attention_gain).astype(jnp.bfloat16)
    query_sum, latent_sum, rotary_sum, square_sum = lax.psum(
        (
            matmul(first_scaled, query_down),
            matmul(first_scaled, latent_down),
            matmul(first_scaled, rotary_down),
            sum_squares(stream_f),
        ),
        ("kv", "tp"),
    )
    first_scale = lax.rsqrt(square_sum / model_width + epsilon)[:, None]
    query_low = first_scale * query_sum
    latent_new = first_scale * latent_sum
    rotary_new = first_scale * rotary_sum
    query_normed = (query_low * inv_rms(query_low)[:, None] * query_gain).astype(jnp.bfloat16)
    latent_row = (latent_new * inv_rms(latent_new)[:, None] * latent_gain).astype(jnp.bfloat16)
    rotary_row = rotate(rotary_new, position).astype(jnp.bfloat16)
    heads_here = key_absorb.shape[0]
    query_plain = matmul(query_normed, query_content).astype(jnp.bfloat16)
    query_plain = query_plain.reshape(batch_rows, heads_here, key_absorb.shape[1])
    query_turned = matmul(query_normed, query_rotary).reshape(
        batch_rows, heads_here, rotary_cache.shape[2]
    )
    query_turned = rotate(query_turned, position).astype(jnp.bfloat16)
    query_latent = jnp.einsum(
        "bhn,hnc->bhc", query_plain, key_absorb, preferred_element_type=jnp.float32
    ).astype(jnp.bfloat16)
    scale = (key_absorb.shape[1] + rotary_cache.shape[2]) ** (-0.5)
    scores = (
        jnp.einsum("bhc,bpc->bhp", query_latent, latent_cache, preferred_element_type=jnp.float32)
        + jnp.einsum("bhr,bpr->bhp", query_turned, rotary_cache, preferred_element_type=jnp.float32)
    ) * scale
    maxima = jnp.max(scores, axis=-1)
    expo = jnp.exp(scores - maxima[..., None])
    totals = jnp.sum(expo, axis=-1)
    weighted = jnp.einsum(
        "bhp,bpc->bhc", expo.astype(jnp.bfloat16), latent_cache, preferred_element_type=jnp.float32
    ).astype(jnp.bfloat16)
    all_maxima, all_totals = (
        lax.all_gather(maxima[None], "kv", axis=0, tiled=True),
        lax.all_gather(totals[None], "kv", axis=0, tiled=True),
    )
    own_score = (
        jnp.sum(
            query_latent.astype(jnp.float32) * latent_row.astype(jnp.float32)[:, None, :], axis=-1
        )
        + jnp.sum(
            query_turned.astype(jnp.float32) * rotary_row.astype(jnp.float32)[:, None, :], axis=-1
        )
    ) * scale
    largest = jnp.maximum(jnp.max(all_maxima, axis=0), own_score)
    factors = jnp.exp(all_maxima - largest[None])
    own_weight = jnp.exp(own_score - largest)
    denominator = jnp.sum(factors * all_totals, axis=0) + own_weight
    merged = jnp.sum(
        factors[..., None]
        * lax.all_gather(weighted[None], "kv", axis=0, tiled=True).astype(jnp.float32),
        axis=0,
    )
    merged = merged + own_weight[..., None] * latent_row.astype(jnp.float32)[:, None, :]
    latent_mix = (merged / denominator[..., None]).astype(jnp.bfloat16)
    head_values = jnp.einsum(
        "bhc,hcv->bhv", latent_mix, value_absorb, preferred_element_type=jnp.float32
    ).astype(jnp.bfloat16)
    head_f = head_values.reshape(batch_rows, heads_here * value_absorb.shape[2]).astype(jnp.float32)
    head_square = lax.psum(sum_squares(head_f), "tp")
    head_scale = lax.rsqrt(head_square / (head_f.shape[1] * tp_count) + epsilon)[:, None]
    head_scaled = (head_f * head_gain).astype(jnp.bfloat16)
    attended = lax.psum(matmul(head_scaled, output_weight).astype(jnp.bfloat16), "tp").astype(
        jnp.float32
    )
    middle = (stream_block.astype(jnp.float32) + head_scale * attended).astype(jnp.bfloat16)
    middle_f = middle.astype(jnp.float32)
    second_scaled = (middle_f * mixer_gain).astype(jnp.bfloat16)
    gate_part = matmul(second_scaled, gate_weight)
    up_part = matmul(second_scaled, up_weight)
    gate_total, up_total, middle_square = (
        lax.psum(gate_part.astype(jnp.bfloat16), "kv").astype(jnp.float32),
        lax.psum(up_part.astype(jnp.bfloat16), "kv").astype(jnp.float32),
        lax.psum(sum_squares(middle_f).astype(jnp.bfloat16), "kv").astype(jnp.float32),
    )
    second_scale = lax.rsqrt(middle_square / model_width + epsilon)[:, None]
    hidden = (jax.nn.silu(second_scale * gate_total) * (second_scale * up_total)).astype(
        jnp.bfloat16
    )
    mixed = lax.psum_scatter(
        matmul(hidden, down_weight).astype(jnp.bfloat16), "tp", scatter_dimension=1, tiled=True
    ).astype(jnp.float32)
    share_width = mixed.shape[1]
    own_middle = lax.dynamic_slice_in_dim(
        middle_f, lax.axis_index("tp") * share_width, share_width, 1
    )
    return (own_middle + mixed).astype(jnp.bfloat16)


LANES = 128
SUBLANES = 8
MESH = pl.DeviceIdType.MESH


def ceil_div(value, step):
    return -(-value // step)


def tables(width, count, position):
    half = width // 2
    freqs = rope_base ** (-np.arange(half, dtype=np.float64) * 2.0 / width)
    angle = position * freqs
    cosine = np.concatenate([np.cos(angle), np.cos(angle)])
    sine = np.concatenate([-np.sin(angle), np.sin(angle)])
    return (
        np.tile(cosine, count)[None].astype(np.float32),
        np.tile(sine, count)[None].astype(np.float32),
    )


def turned(values, cosine, sine, width):
    lanes = values.shape[1]
    half = width // 2
    lane = lax.broadcasted_iota(jnp.int32, values.shape, 1)
    ahead = pltpu.roll(values, lanes - half, 1)
    behind = pltpu.roll(values, half, 1)
    swapped = jnp.where(lax.rem(lane, width) < half, ahead, behind)
    return values * cosine + swapped * sine


def split_sum(values, lanes):
    high = values.astype(jnp.bfloat16).astype(jnp.float32)
    lane = lax.broadcasted_iota(jnp.int32, (values.shape[0], lanes), 1)
    return jnp.where(lane < lanes // 2, high, values - high).astype(jnp.bfloat16)


def joined_sum(parts, lanes):
    half = lanes // 2
    return parts[:, 0:1] + parts[:, half : half + 1]


def matmul_nt(left, right):
    return lax.dot_general(
        left, right, (((1,), (1,)), ((), ())), preferred_element_type=jnp.float32
    )


def fused(
    n_kv,
    n_tp,
    dims,
    stream_ref,
    attention_gain,
    query_gain,
    latent_gain,
    head_gain,
    mixer_gain,
    cos_ref,
    sin_ref,
    *refs,
):
    rows, depth, qrank, kvrank, rope, nope, vdim, heads, hidden_width, block_width, share, positions = dims
    hbm = refs[:13]
    out_ref = refs[13]
    vmem = refs[14:27]
    (
        load_sems,
        tp_sems,
        kv_sems,
        stream_all,
        a_send,
        a_recv,
        a_sum,
        a_part,
        a_total,
        a_all,
        q_lat,
        q_rot,
        own_lat,
        own_stat,
        own_rows,
        s_ref,
        e_ref,
        w_ref,
        w_send,
        w_recv,
        st_send,
        st_recv,
        hv_send,
        hv_recv,
        hv_rows,
        o_recv,
        o_send,
        mid_ref,
        d_send,
        d_recv,
        h_all,
        h_send,
        e_send,
        e_recv,
    ) = refs[27:]
    (
        qd_v,
        ld_v,
        rd_v,
        qc_v,
        qr_v,
        ka_v,
        lat_v,
        rot_v,
        va_v,
        ow_v,
        gate_v,
        up_v,
        down_v,
    ) = vmem
    kv = lax.axis_index("kv")
    tp = lax.axis_index("tp")
    model_width = block_width * n_kv

    loads = []
    for index, (source, target) in enumerate(zip(hbm, vmem)):
        if index in (10, 11):
            target = target.at[:, pl.ds(0, hidden_width)]
        elif index == 12:
            target = target.at[pl.ds(0, hidden_width)]
        copy = pltpu.make_async_copy(source, target, load_sems.at[index])
        copy.start()
        loads.append(copy)

    barrier = pltpu.get_barrier_semaphore()
    for d in range(1, n_tp):
        pl.semaphore_signal(
            barrier, inc=1, device_id=(kv, lax.rem(tp + d, n_tp)), device_id_type=MESH
        )
    for d in range(1, n_kv):
        pl.semaphore_signal(
            barrier, inc=1, device_id=(lax.rem(kv + d, n_kv), tp), device_id_type=MESH
        )

    sent = []

    def send(axis, stage, d, source, target):
        if axis == "tp":
            peer, sems = (kv, lax.rem(tp + d, n_tp)), tp_sems
        else:
            peer, sems = (lax.rem(kv + d, n_kv), tp), kv_sems
        copy = pltpu.make_async_remote_copy(
            src_ref=source,
            dst_ref=target,
            send_sem=sems.at[stage, 0, d - 1],
            recv_sem=sems.at[stage, 1, d - 1],
            device_id=peer,
            device_id_type=MESH,
        )
        copy.start()
        sent.append(copy)
        return copy

    def arrive(copies):
        for copy in copies:
            copy.wait_recv()

    pad = gate_v.shape[1] - hidden_width
    if pad:
        gate_v[:, hidden_width:] = jnp.zeros((block_width, pad), gate_v.dtype)
        up_v[:, hidden_width:] = jnp.zeros((block_width, pad), up_v.dtype)
        down_v[hidden_width:, :] = jnp.zeros((pad, block_width), down_v.dtype)

    stream_f = stream_ref[...].astype(jnp.float32)
    first_scaled = (stream_f * attention_gain[...]).astype(jnp.bfloat16)
    for index in range(3):
        loads[index].wait()
    parts = [matmul(first_scaled, qd_v[...]), matmul(first_scaled, ld_v[...])]
    rotary_part = matmul_nt(first_scaled, rd_v[...])
    square = jnp.sum(stream_f * stream_f, axis=1, keepdims=True)
    last = jnp.concatenate(
        [rotary_part, jnp.broadcast_to(square, (rows, LANES - rope))], axis=1
    )
    tiles = []
    for part in parts:
        for j in range(part.shape[1] // LANES):
            tiles.append(part[:, j * LANES : (j + 1) * LANES])
    tiles.append(last)
    row_tiles = rows // SUBLANES
    blocks = a_send.shape[1]
    per_kv = blocks // n_kv
    for t in range(n_tp):
        for i in range(blocks):
            k, r = divmod(i, row_tiles)
            j = k * n_tp + t
            if j < len(tiles):
                a_send[t, i] = tiles[j][r * SUBLANES : (r + 1) * SUBLANES].astype(jnp.bfloat16)
            else:
                a_send[t, i] = jnp.zeros((SUBLANES, LANES), jnp.bfloat16)
    pl.semaphore_wait(barrier, n_tp - 1 + n_kv - 1)
    copies = [
        send("tp", 1, d, a_send.at[lax.rem(tp + d, n_tp)], a_recv.at[tp]) for d in range(1, n_tp)
    ]
    a_recv[tp] = a_send[tp]
    arrive(copies)
    total = a_recv[0].astype(jnp.float32)
    for t in range(1, n_tp):
        total = total + a_recv[t].astype(jnp.float32)
    a_sum[...] = total.astype(jnp.bfloat16)
    copies = [
        send(
            "kv",
            0,
            d,
            a_sum.at[pl.ds(lax.rem(kv + d, n_kv) * per_kv, per_kv)],
            a_part.at[kv],
        )
        for d in range(1, n_kv)
    ]
    stream_copies = [send("tp", 0, d, stream_ref, stream_all.at[tp]) for d in range(1, n_tp)]
    stream_all[tp] = stream_ref[...]
    a_part[kv] = a_sum[pl.ds(kv * per_kv, per_kv)]
    arrive(copies)
    total = a_part[0].astype(jnp.float32)
    for p in range(1, n_kv):
        total = total + a_part[p].astype(jnp.float32)
    a_total[pl.ds(kv * per_kv, per_kv)] = total.astype(jnp.bfloat16)
    mine = a_total.at[pl.ds(kv * per_kv, per_kv)]
    arrive([send("kv", 1, d, mine, mine) for d in range(1, n_kv)])
    copies = [send("tp", 2, d, a_total, a_all.at[tp]) for d in range(1, n_tp)]
    a_all[tp] = a_total[...]
    arrive(copies)

    def tile_of(j):
        k, t = divmod(j, n_tp)
        return jnp.concatenate([a_all[t, k * row_tiles + r].astype(jnp.float32) for r in range(row_tiles)], axis=0)

    q_tiles, l_tiles = qrank // LANES, kvrank // LANES
    last = tile_of(q_tiles + l_tiles)
    first_scale = lax.rsqrt(last[:, rope : rope + 1] / model_width + epsilon)
    query_low = first_scale * jnp.concatenate([tile_of(j) for j in range(q_tiles)], axis=1)
    latent_new = first_scale * jnp.concatenate(
        [tile_of(q_tiles + j) for j in range(l_tiles)], axis=1
    )

    def normed(values, gain):
        mean = jnp.sum(values * values, axis=1, keepdims=True) / values.shape[1]
        return (values * lax.rsqrt(mean + epsilon) * gain).astype(jnp.bfloat16)

    gain = jnp.concatenate([query_gain[j : j + 1] for j in range(q_tiles)], axis=1)
    query_normed = normed(query_low, gain)
    latent_row = normed(latent_new, latent_gain[...]).astype(jnp.float32)
    lane = lax.broadcasted_iota(jnp.int32, (rows, LANES), 1)
    cosine, sine = cos_ref[...], sin_ref[...]
    rotary_row = turned(first_scale * last, cosine[:, :LANES], sine[:, :LANES], rope)
    rotary_row = jnp.where(lane < rope, rotary_row, 0.0).astype(jnp.bfloat16).astype(jnp.float32)

    loads[3].wait()
    query_plain = matmul(query_normed, qc_v[...]).astype(jnp.bfloat16)
    loads[4].wait()
    query_turned = turned(matmul(query_normed, qr_v[...]), cosine, sine, rope)
    query_turned = query_turned.astype(jnp.bfloat16).astype(jnp.float32)
    loads[5].wait()
    scale = (nope + rope) ** (-0.5)
    per_tile = LANES // rope
    for h in range(heads):
        row = pl.ds(h, rows, stride=heads)
        latent = matmul(query_plain[:, h * nope : (h + 1) * nope], ka_v[h])
        latent = latent.astype(jnp.bfloat16).astype(jnp.float32)
        tile = h // per_tile
        rotary = query_turned[:, tile * LANES : (tile + 1) * LANES]
        shift = (h % per_tile) * rope
        if shift:
            rotary = pltpu.roll(rotary, LANES - shift, 1)
        rotary = jnp.where(lane < rope, rotary, 0.0)
        own = (
            jnp.sum(latent * latent_row, axis=1, keepdims=True)
            + jnp.sum(rotary * rotary_row, axis=1, keepdims=True)
        ) * scale
        for c in range(l_tiles):
            q_lat[c, row, :] = latent[:, c * LANES : (c + 1) * LANES]
            own_lat[c, row, :] = latent_row[:, c * LANES : (c + 1) * LANES]
        q_rot[row, :] = rotary
        own_stat[row, :] = jnp.broadcast_to(own, (rows, LANES))

    group = SUBLANES // heads
    steps = rows // group
    unroll = 3 if steps % 3 == 0 else 1
    sub_row = lax.broadcasted_iota(jnp.int32, (SUBLANES, 1), 0) // heads
    loads[6].wait()
    loads[7].wait()

    def score_step(outer, carry):
        for inner in range(unroll):
            i = outer * unroll + inner
            at = pl.ds(pl.multiple_of(i * SUBLANES, SUBLANES), SUBLANES)
            query = jnp.concatenate([q_lat[c, at, :] for c in range(l_tiles)], axis=1).astype(
                jnp.bfloat16
            )
            rotary = q_rot[at, :][:, :rope].astype(jnp.bfloat16)
            result = None
            for s in range(group):
                b = i * group + s
                score = matmul_nt(query, lat_v[b]) + matmul(rotary, rot_v[b])
                result = score if s == 0 else jnp.where(sub_row == s, score, result)
            s_ref[at, :] = result * scale
        return carry

    lax.fori_loop(0, steps // unroll, score_step, 0)
    scores = s_ref[...]
    maxima = jnp.max(scores, axis=1, keepdims=True)
    expo = jnp.exp(scores - maxima)
    totals = jnp.sum(expo, axis=1, keepdims=True)
    e_ref[...] = expo
    all_rows = rows * heads
    own_rows_count = all_rows // n_kv
    stat_lane = lax.broadcasted_iota(jnp.int32, (all_rows, LANES), 1)
    stats = jnp.where(stat_lane < LANES // 2, maxima, totals)
    for p in range(n_kv):
        st_send[p] = stats[p * own_rows_count : (p + 1) * own_rows_count]
    stat_copies = [
        send("kv", 2, d, st_send.at[lax.rem(kv + d, n_kv)], st_recv.at[kv])
        for d in range(1, n_kv)
    ]
    st_recv[kv] = st_send[kv]

    def weight_step(outer, carry):
        for inner in range(unroll):
            i = outer * unroll + inner
            at = pl.ds(pl.multiple_of(i * SUBLANES, SUBLANES), SUBLANES)
            weights = e_ref[at, :].astype(jnp.bfloat16)
            result = None
            for s in range(group):
                value = matmul(weights, lat_v[i * group + s])
                result = value if s == 0 else jnp.where(sub_row == s, value, result)
            w_ref[at, :] = result
        return carry

    lax.fori_loop(0, steps // unroll, weight_step, 0)
    for p in range(n_kv):
        own = slice(p * own_rows_count, (p + 1) * own_rows_count)
        w_send[p] = w_ref[own, :].astype(jnp.bfloat16)
        for c in range(l_tiles):
            own_rows[p, :, c * LANES : (c + 1) * LANES] = own_lat[c, own, :]
        own_rows[p, :, kvrank:] = own_stat[own, :]
    copies = [
        send("kv", 3, d, w_send.at[lax.rem(kv + d, n_kv)], w_recv.at[kv]) for d in range(1, n_kv)
    ]
    w_recv[kv] = w_send[kv]
    own = own_rows[kv]
    own_score = own[:, kvrank : kvrank + 1]
    arrive(stat_copies)
    stat = [st_recv[p] for p in range(n_kv)]
    largest = own_score
    for p in range(n_kv):
        largest = jnp.maximum(largest, stat[p][:, 0:1])
    own_weight = jnp.exp(own_score - largest)
    denominator = own_weight
    factors = []
    for p in range(n_kv):
        factor = jnp.exp(stat[p][:, 0:1] - largest)
        factors.append(factor)
        denominator = denominator + factor * stat[p][:, LANES // 2 : LANES // 2 + 1]
    arrive(copies)
    merged = own_weight * own[:, :kvrank]
    for p in range(n_kv):
        merged = merged + factors[p] * w_recv[p].astype(jnp.float32)
    latent_mix = (merged / denominator).astype(jnp.bfloat16)
    loads[8].wait()
    head_row = lax.rem(lax.broadcasted_iota(jnp.int32, (own_rows_count, 1), 0), heads)
    values = None
    for h in range(heads):
        value = matmul(latent_mix, va_v[h])
        values = value if h == 0 else jnp.where(head_row == h, value, values)
    values = values.astype(jnp.bfloat16)
    hv_send[...] = values
    copies = [send("kv", 4, d, hv_send, hv_recv.at[kv]) for d in range(1, n_kv)]
    hv_recv[kv] = values
    arrive(copies)
    for p in range(n_kv):
        hv_rows[p * own_rows_count : (p + 1) * own_rows_count, :] = hv_recv[p].astype(jnp.float32)
    head_f = jnp.concatenate(
        [hv_rows[pl.ds(h, rows, stride=heads), :] for h in range(heads)], axis=1
    )
    head_square = jnp.sum(head_f * head_f, axis=1, keepdims=True)
    head_scaled = (head_f * head_gain[...]).astype(jnp.bfloat16)
    loads[9].wait()
    o_send[:, :block_width] = matmul(head_scaled, ow_v[...]).astype(jnp.bfloat16)
    o_send[:, block_width:] = split_sum(head_square, LANES)
    copies = [send("tp", 4, d, o_send, o_recv.at[tp]) for d in range(1, n_tp)]
    o_recv[tp] = o_send[...]
    arrive(stream_copies)
    stream_block = jnp.concatenate([stream_all[t] for t in range(n_tp)], axis=1).astype(
        jnp.float32
    )
    arrive(copies)
    attended = o_recv[0].astype(jnp.float32)
    for t in range(1, n_tp):
        attended = attended + o_recv[t].astype(jnp.float32)
    square = joined_sum(attended[:, block_width:], LANES)
    attended = attended[:, :block_width]
    head_scale = lax.rsqrt(square / (heads * vdim * n_tp) + epsilon)
    middle = (stream_block + head_scale * attended).astype(jnp.bfloat16).astype(jnp.float32)
    for t in range(n_tp):
        mid_ref[t] = middle[:, t * share : (t + 1) * share]

    square = split_sum(jnp.sum(middle * middle, axis=1, keepdims=True), LANES)
    second_scaled = (middle * mixer_gain[...]).astype(jnp.bfloat16)
    loads[10].wait()
    loads[11].wait()
    chunk = gate_v.shape[1] // n_kv
    copies = []
    far_first = sorted(range(1, n_kv), key=lambda d: abs(2 * d - n_kv)) + [0]
    for d in far_first:
        peer = lax.rem(kv + d, n_kv)
        columns = pl.ds(pl.multiple_of(peer * chunk, LANES), chunk)
        gate = matmul(second_scaled, gate_v[:, columns]).astype(jnp.bfloat16)
        up = matmul(second_scaled, up_v[:, columns]).astype(jnp.bfloat16)
        if d:
            d_send[peer, :, :chunk] = gate
            d_send[peer, :, chunk : 2 * chunk] = up
            d_send[peer, :, 2 * chunk :] = square
            copies.append(send("kv", 6, d, d_send.at[peer], d_recv.at[kv]))
        else:
            d_recv[kv, :, :chunk] = gate
            d_recv[kv, :, chunk : 2 * chunk] = up
            d_recv[kv, :, 2 * chunk :] = square
    arrive(copies)
    total = d_recv[0].astype(jnp.float32)
    for p in range(1, n_kv):
        total = total + d_recv[p].astype(jnp.float32)
    square = joined_sum(total[:, 2 * chunk :], LANES)
    second_scale = lax.rsqrt(square / model_width + epsilon)
    gate = second_scale * total[:, :chunk]
    up = second_scale * total[:, chunk : 2 * chunk]
    h_send[...] = (gate / (1.0 + jnp.exp(-gate)) * up).astype(jnp.bfloat16)
    copies = [send("kv", 7, d, h_send, h_all.at[kv]) for d in range(1, n_kv)]
    loads[12].wait()
    mixed = matmul(h_send[...], down_v[pl.ds(pl.multiple_of(kv * chunk, LANES), chunk), :])
    for d in range(1, n_kv):
        copies[d - 1].wait_recv()
        peer = lax.rem(kv + n_kv - d, n_kv)
        mixed = mixed + matmul(
            h_all[peer], down_v[pl.ds(pl.multiple_of(peer * chunk, LANES), chunk), :]
        )
    for t in range(n_tp):
        e_send[t] = mixed[:, t * share : (t + 1) * share].astype(jnp.bfloat16)
    copies = [
        send("tp", 5, d, e_send.at[lax.rem(tp + d, n_tp)], e_recv.at[tp]) for d in range(1, n_tp)
    ]
    e_recv[tp] = e_send[tp]
    arrive(copies)
    total = e_recv[0].astype(jnp.float32)
    for t in range(1, n_tp):
        total = total + e_recv[t].astype(jnp.float32)
    out_ref[...] = (mid_ref[tp] + total).astype(jnp.bfloat16)
    for copy in sent:
        copy.wait_send()


def layer(
    n_kv,
    n_tp,
    stream,
    attention_gain,
    query_down,
    latent_down,
    rotary_down,
    query_gain,
    latent_gain,
    query_content,
    query_rotary,
    key_absorb,
    value_absorb,
    latent_cache,
    rotary_cache,
    head_gain,
    output_weight,
    mixer_gain,
    gate_weight,
    up_weight,
    down_weight,
):
    rows, share = stream.shape
    heads, nope, kvrank = key_absorb.shape
    vdim = value_absorb.shape[2]
    qrank = query_down.shape[1]
    rope = rotary_down.shape[1]
    positions = latent_cache.shape[1]
    block_width, hidden_width = gate_weight.shape
    aligned = (
        all(
            size % LANES == 0
            for size in (share, qrank, kvrank, nope, vdim, positions, hidden_width)
        )
        and rope < LANES
        and LANES % rope == 0
        and (heads * rope) % LANES == 0
        and rows % SUBLANES == 0
        and SUBLANES % heads == 0
        and rows % (SUBLANES // heads) == 0
        and rows % n_kv == 0
        and n_kv > 1
        and n_tp > 1
    )
    if not aligned:
        return local(
            stream,
            attention_gain,
            query_down,
            latent_down,
            rotary_down,
            query_gain,
            latent_gain,
            query_content,
            query_rotary,
            key_absorb,
            value_absorb,
            latent_cache,
            rotary_cache,
            head_gain,
            output_weight,
            mixer_gain,
            gate_weight,
            up_weight,
            down_weight,
        )
    dims = (rows, share, qrank, kvrank, rope, nope, vdim, heads, hidden_width, block_width, share, positions)
    cosine, sine = tables(rope, heads, positions * n_kv)
    n_tiles = qrank // LANES + kvrank // LANES + 1
    blocks = ceil_div(ceil_div(n_tiles, n_tp) * (rows // SUBLANES), n_kv) * n_kv
    chunk = ceil_div(ceil_div(hidden_width, LANES), n_kv) * LANES
    all_rows = rows * heads
    own = all_rows // n_kv
    l_tiles = kvrank // LANES
    bf16, f32 = jnp.bfloat16, jnp.float32
    big = (
        query_down,
        latent_down,
        rotary_down.T,
        query_content,
        query_rotary,
        key_absorb,
        latent_cache,
        jnp.swapaxes(rotary_cache, 1, 2),
        value_absorb,
        output_weight,
        gate_weight,
        up_weight,
        down_weight,
    )
    held = [pltpu.VMEM(array.shape, array.dtype) for array in big]
    held[10] = held[11] = pltpu.VMEM((block_width, chunk * n_kv), bf16)
    held[12] = pltpu.VMEM((chunk * n_kv, block_width), bf16)
    scratch = held + [
        pltpu.SemaphoreType.DMA((len(big),)),
        pltpu.SemaphoreType.DMA((6, 2, n_tp - 1)),
        pltpu.SemaphoreType.DMA((8, 2, n_kv - 1)),
        pltpu.VMEM((n_tp, rows, share), bf16),
        pltpu.VMEM((n_tp, blocks, SUBLANES, LANES), bf16),
        pltpu.VMEM((n_tp, blocks, SUBLANES, LANES), bf16),
        pltpu.VMEM((blocks, SUBLANES, LANES), bf16),
        pltpu.VMEM((n_kv, blocks // n_kv, SUBLANES, LANES), bf16),
        pltpu.VMEM((blocks, SUBLANES, LANES), bf16),
        pltpu.VMEM((n_tp, blocks, SUBLANES, LANES), bf16),
        pltpu.VMEM((l_tiles, all_rows, LANES), f32),
        pltpu.VMEM((all_rows, LANES), f32),
        pltpu.VMEM((l_tiles, all_rows, LANES), f32),
        pltpu.VMEM((all_rows, LANES), f32),
        pltpu.VMEM((n_kv, own, kvrank + LANES), f32),
        pltpu.VMEM((all_rows, positions), f32),
        pltpu.VMEM((all_rows, positions), f32),
        pltpu.VMEM((all_rows, kvrank), f32),
        pltpu.VMEM((n_kv, own, kvrank), bf16),
        pltpu.VMEM((n_kv, own, kvrank), bf16),
        pltpu.VMEM((n_kv, own, LANES), f32),
        pltpu.VMEM((n_kv, own, LANES), f32),
        pltpu.VMEM((own, vdim), bf16),
        pltpu.VMEM((n_kv, own, vdim), bf16),
        pltpu.VMEM((all_rows, vdim), f32),
        pltpu.VMEM((n_tp, rows, block_width + LANES), bf16),
        pltpu.VMEM((rows, block_width + LANES), bf16),
        pltpu.VMEM((n_tp, rows, share), f32),
        pltpu.VMEM((n_kv, rows, 2 * chunk + LANES), bf16),
        pltpu.VMEM((n_kv, rows, 2 * chunk + LANES), bf16),
        pltpu.VMEM((n_kv, rows, chunk), bf16),
        pltpu.VMEM((rows, chunk), bf16),
        pltpu.VMEM((n_tp, rows, share), bf16),
        pltpu.VMEM((n_tp, rows, share), bf16),
    ]
    vmem = pl.BlockSpec(memory_space=pltpu.VMEM)
    return pl.pallas_call(
        functools.partial(fused, n_kv, n_tp, dims),
        out_shape=jax.ShapeDtypeStruct(stream.shape, stream.dtype),
        in_specs=[vmem] * 8 + [pl.BlockSpec(memory_space=pl.ANY)] * len(big),
        out_specs=vmem,
        scratch_shapes=scratch,
        compiler_params=pltpu.CompilerParams(
            collective_id=0, has_side_effects=True, vmem_limit_bytes=64000000
        ),
        name="layer",
    )(
        stream,
        attention_gain[None],
        query_gain.reshape(qrank // LANES, LANES),
        latent_gain[None],
        head_gain[None],
        mixer_gain[None],
        cosine,
        sine,
        *big,
    )


def solution(mesh):
    return jax.shard_map(
        functools.partial(layer, mesh.shape["kv"], mesh.shape["tp"]),
        mesh=mesh,
        in_specs=(
            P(None, ("kv", "tp")),
            P(("kv", "tp")),
            P(("kv", "tp"), None),
            P(("kv", "tp"), None),
            P(("kv", "tp"), None),
            P(),
            P(),
            P(None, "tp"),
            P(None, "tp"),
            P("tp", None, None),
            P("tp", None, None),
            P(None, "kv", None),
            P(None, "kv", None),
            P("tp"),
            P("tp", "kv"),
            P("kv"),
            P("kv", "tp"),
            P("kv", "tp"),
            P("tp", "kv"),
        ),
        out_specs=P(None, ("kv", "tp")),
        check_vma=False,
    )
```
